32 devices in a mesh: grp: 1, fs: 2 (over x), tp: 16 (over z, y, core).
Axes of the slice: x: 2, y: 2, z: 4, core: 2. Of those that a mesh axis runs over, the one named last changes fastest.
Arguments:
- prompt_rows: bfloat16 [512, 2048], P(('grp', 'fs')), may hold values from -6 to 6
- gain_before: float32 [2048], P('fs'), may hold values from 0.1 to 1.9
- gate_before: float32 [2048, 5632], P('fs', 'tp'), may hold values from -0.125 to 0.125
- up_before: float32 [2048, 5632], P('fs', 'tp'), may hold values from -0.125 to 0.125
- down_before: float32 [5632, 2048], P('fs', 'tp'), may hold values from -0.3125 to 0.3125
- gain_after: float32 [2048], P('fs'), may hold values from 0.1 to 1.9
- gate_after: float32 [2048, 5632], P('fs', 'tp'), may hold values from -0.125 to 0.125
- up_after: float32 [2048, 5632], P('fs', 'tp'), may hold values from -0.125 to 0.125
- down_after: float32 [5632, 2048], P('fs', 'tp'), may hold values from -0.3125 to 0.3125
Outputs:
- mixed_rows: bfloat16 [512, 2048], P(('grp', 'fs'))
- served_gate_before: bfloat16 [2048, 5632], P('grp', 'tp')
- served_up_before: bfloat16 [2048, 5632], P('grp', 'tp')
- served_down_before: bfloat16 [5632, 2048], P(('grp', 'tp'))
- served_gate_after: bfloat16 [2048, 5632], P('grp', 'tp')
- served_up_after: bfloat16 [2048, 5632], P('grp', 'tp')
- served_down_after: bfloat16 [5632, 2048], P(('grp', 'tp'))
The draws below stay inside these ranges and needn't reach their ends.
All inputs are finite; a program needn't handle non-finite values.
Results may differ from the reference program's by a relative error of at most 0.03.
Values may be sent and summed in bfloat16 or wider, within the bound.
A program may use at most 64 MiB of HBM per device.

```python
import jax
import jax.numpy as jnp
from jax import lax

D = 2048
FF = 5632
TOKENS = 512
N_TP = 16


def levels(own_key, extent, cuts, least, largest):
    level, own = 1.0, jax.random.fold_in(own_key, 6)
    for position, shards_of in cuts:
        draws = jnp.exp(jax.random.uniform(jax.random.fold_in(own, position), (shards_of,), jnp.float32, least / len(cuts), largest / len(cuts)))
        level = level * jnp.repeat(draws, extent[position] // shards_of).reshape([-1 if axis == position else 1 for axis in range(len(extent))])
    return level


def scatter_about(rng, extent, spread, bound, pieces=(), kind=jnp.bfloat16):
    entries = spread * jax.random.normal(rng, extent, jnp.float32)
    if pieces:
        entries = entries * levels(rng, extent, pieces, -0.22, 0.18)
    return jnp.clip(entries, -bound, bound).astype(kind)


def setup_inputs(seed: int = 0, part: int = 0) -> dict:
    key_list = jax.random.split(jax.random.key(seed), 10)
    part_splits = jax.random.split(jax.random.fold_in(key_list[9], part), 10)
    return {
        "prompt_rows": scatter_about(part_splits[0], (TOKENS, D), 1.0, 6.0, ((0, 2),)),
        "gain_before": jnp.clip(1.0 + 0.18 * jax.random.normal(key_list[1], (D,), jnp.float32), 0.1, 1.9),
        "gate_before": scatter_about(key_list[2], (D, FF), D ** -0.5, 0.125, ((0, 2), (1, 16)), jnp.float32),
        "up_before": scatter_about(key_list[3], (D, FF), D ** -0.5, 0.125, ((0, 2), (1, 16)), jnp.float32),
        "down_before": scatter_about(key_list[4], (FF, D), (FF // 16) ** -0.5, 0.3125, ((0, 2), (1, 16)), jnp.float32),
        "gain_after": jnp.clip(1.0 + 0.18 * jax.random.normal(key_list[5], (D,), jnp.float32), 0.1, 1.9),
        "gate_after": scatter_about(key_list[6], (D, FF), D ** -0.5, 0.125, ((0, 2), (1, 16)), jnp.float32),
        "up_after": scatter_about(key_list[7], (D, FF), D ** -0.5, 0.125, ((0, 2), (1, 16)), jnp.float32),
        "down_after": scatter_about(key_list[8], (FF, D), (FF // 16) ** -0.5, 0.3125, ((0, 2), (1, 16)), jnp.float32),
    }


EPS = 1e-06

def fold(gain, gate_w, up_w, down_w):
    served_gate = (gain[:, None] * gate_w).astype(jnp.bfloat16)
    served_up = (gain[:, None] * up_w).astype(jnp.bfloat16)
    return (served_gate, served_up, down_w.astype(jnp.bfloat16))

def half_step(row_block, gate_w, up_w, down_w):
    values = row_block.astype(jnp.float32)
    normed = (values * lax.rsqrt(lax.optimization_barrier(jnp.mean(values * values, axis=-1, keepdims=True)) + EPS)).astype(jnp.bfloat16)
    gate_pre = jnp.dot(normed, gate_w, preferred_element_type=jnp.float32)
    up_pre = jnp.dot(normed, up_w, preferred_element_type=jnp.float32)
    hidden = (jax.nn.silu(gate_pre) * up_pre).astype(jnp.bfloat16)
    width = FF // N_TP
    hidden_blocks = hidden.reshape(hidden.shape[0], N_TP, width).transpose(1, 0, 2)
    down_blocks = down_w.reshape(N_TP, width, D)

    def add_block(total, pair):
        part_sum = jnp.dot(pair[0], pair[1], preferred_element_type=jnp.float32).astype(jnp.bfloat16)
        part_sum = lax.optimization_barrier(part_sum)
        return (total + part_sum.astype(jnp.float32), None)
    total, _ = lax.scan(add_block, jnp.zeros((hidden.shape[0], D), jnp.float32), (hidden_blocks, down_blocks))
    return (values + 0.5 * total).astype(jnp.bfloat16)

def reference(prompt_rows, gain_before, gate_before, up_before, down_before, gain_after, gate_after, up_after, down_after):
    gate_one, up_one, down_one = fold(gain_before, gate_before, up_before, down_before)
    gate_two, up_two, down_two = fold(gain_after, gate_after, up_after, down_after)
    middle = half_step(prompt_rows, gate_one, up_one, down_one)
    mixed = half_step(middle, gate_two, up_two, down_two)
    return (mixed, gate_one, up_one, down_one, gate_two, up_two, down_two)
```

```python
import functools

import jax
import jax.numpy as jnp
from jax import lax
from jax.experimental import pallas as pl
from jax.experimental.pallas import tpu as pltpu
from jax.sharding import PartitionSpec as P

MESH = pl.DeviceIdType.MESH
BF16 = jnp.bfloat16
F32 = jnp.float32

EPS = 1e-06


def serve_weights(gain, gate_w, up_w, down_w):
    gate_half = (gain[:, None] * gate_w).astype(jnp.bfloat16)
    up_half = (gain[:, None] * up_w).astype(jnp.bfloat16)
    down_half = down_w.astype(jnp.bfloat16)
    gate_whole, up_whole = (
        lax.all_gather(gate_half, "fs", axis=0, tiled=True),
        lax.all_gather(up_half, "fs", axis=0, tiled=True),
    )
    tall_block = lax.all_gather(down_half, "fs", axis=0, tiled=True)
    down_whole = lax.all_to_all(tall_block, "tp", split_axis=0, concat_axis=1, tiled=True)
    return (gate_whole, up_whole, down_whole)


def half_step(row_block, gate_w, up_w, down_w):
    values = row_block.astype(jnp.float32)
    normed = (values * lax.rsqrt(jnp.mean(values * values, axis=-1, keepdims=True) + EPS)).astype(
        jnp.bfloat16
    )
    gate_pre = jnp.dot(normed, gate_w, preferred_element_type=jnp.float32)
    up_pre = jnp.dot(normed, up_w, preferred_element_type=jnp.float32)
    hidden = (jax.nn.silu(gate_pre) * up_pre).astype(jnp.bfloat16)
    total = lax.psum(
        jnp.dot(hidden, down_w, preferred_element_type=jnp.float32).astype(jnp.bfloat16), "tp"
    ).astype(jnp.float32)
    return (values + 0.5 * total).astype(jnp.bfloat16)


def body(
    prompt_rows,
    gain_before,
    gate_before,
    up_before,
    down_before,
    gain_after,
    gate_after,
    up_after,
    down_after,
):
    gate_one, up_one, down_one = serve_weights(gain_before, gate_before, up_before, down_before)
    gate_two, up_two, down_two = serve_weights(gain_after, gate_after, up_after, down_after)
    middle = half_step(prompt_rows, gate_one, up_one, down_one)
    mixed = half_step(middle, gate_two, up_two, down_two)
    return (mixed, gate_one, up_one, down_one, gate_two, up_two, down_two)


def rows_of(start, size, unit):
    return pl.ds(pl.multiple_of(start, unit), size)


def kernel(
    n_tp,
    x_hbm, gain1_hbm, gate1_hbm, up1_hbm, down1_hbm, gain2_hbm, gate2_hbm, up2_hbm, down2_hbm,
    mixed_hbm, gate1_out, up1_out, down1_out, gate2_out, up2_out, down2_out,
    x, gain, wide, tall_in, served, tall, down, normed, hidden, part, pair, half, scatter, rows_out,
    in_sem, out_sem, x_send, x_recv, a_send, a_recv, p_send, p_recv, s_send, s_recv, g_send, g_recv,
    h_send, h_recv,
):
    f = lax.axis_index("fs")
    t = lax.axis_index("tp")
    other = 1 - f
    core = lax.rem(t, 2)
    chip = t // 2
    sibling = t + 1 - 2 * core
    chips = n_tp // 2
    depth = wide.shape[1]
    tall_half = tall_in.shape[1]
    block = down.shape[1]
    col = tall.shape[2]
    tokens = x.shape[0]
    side = tokens // 2
    piece = side // chips
    per_half = n_tp // 2

    loads = {}
    sources = (
        ("down1", down1_hbm, tall_in.at[0]), ("gain1", gain1_hbm, gain.at[0]),
        ("gate1", gate1_hbm, wide.at[0]), ("up1", up1_hbm, wide.at[1]),
        ("down2", down2_hbm, tall_in.at[1]), ("gain2", gain2_hbm, gain.at[1]),
        ("gate2", gate2_hbm, wide.at[2]), ("up2", up2_hbm, wide.at[3]), ("x", x_hbm, x),
    )
    for i, (name, src, dst) in enumerate(sources):
        loads[name] = pltpu.make_async_copy(src, dst, in_sem.at[i])
        loads[name].start()

    barrier = pltpu.get_barrier_semaphore()
    for k in range(1, n_tp):
        pl.semaphore_signal(
            barrier, inc=1, device_id={"fs": f, "tp": lax.rem(t + k, n_tp)}, device_id_type=MESH
        )
    pl.semaphore_signal(barrier, inc=1, device_id={"fs": other, "tp": t}, device_id_type=MESH)
    pl.semaphore_wait(barrier, n_tp)

    def across(ref, slot):
        return pltpu.make_async_remote_copy(
            src_ref=ref, dst_ref=ref, send_sem=x_send.at[slot], recv_sem=x_recv.at[slot],
            device_id={"fs": other, "tp": t}, device_id_type=MESH,
        )

    def fold_wide(i, gain_slot):
        step = depth // 8

        def one(k, _):
            rows = rows_of(k * step, step, step)
            value = gain[gain_slot, rows, :] * wide[i, rows, :]
            served[i, rows_of(f * depth + k * step, step, step), :] = value.astype(BF16)
            return 0

        lax.fori_loop(0, 8, one, 0)
        sent = across(served.at[i, rows_of(f * depth, depth, depth)], i)
        sent.start()
        return sent

    def fold_tall(layer):
        step = tall_half // 8

        def one(k, _):
            tall[layer, rows_of(f * tall_half + k * step, step, 16), :] = tall_in[
                layer, rows_of(k * step, step, 16), :
            ].astype(BF16)
            return 0

        lax.fori_loop(0, 8, one, 0)
        sent = across(tall.at[layer, rows_of(f * tall_half, tall_half, 16)], 4 + layer)
        sent.start()
        return sent

    my_cols = pl.ds(pl.multiple_of(t * col, col), col)

    def block_copy(layer, b, sender):
        return pltpu.make_async_remote_copy(
            src_ref=tall.at[layer, rows_of(b * block, block, 16)],
            dst_ref=down.at[layer, :, my_cols],
            send_sem=a_send.at[layer, b], recv_sem=a_recv.at[layer, sender],
            device_id={"fs": f, "tp": b}, device_id_type=MESH,
        )

    def hand_out(layer, which):
        def one(k, _):
            b = which * per_half + lax.rem(t + k, per_half)

            @pl.when(b != t)
            def _():
                block_copy(layer, b, t).start()

            return 0

        lax.fori_loop(0, per_half, one, 0)

    def collect(layer):
        def one(k, _):
            block_copy(layer, t, lax.rem(t + k, n_tp)).wait_recv()
            return 0

        lax.fori_loop(1, n_tp, one, 0)
        down[layer, :, my_cols] = tall[layer, rows_of(t * block, block, 16), :]

    outs = []

    def put(src, dst):
        copy = pltpu.make_async_copy(src, dst, out_sem.at[len(outs)])
        copy.start()
        outs.append(copy)

    sends = []
    loads["down1"].wait()
    tall_one = fold_tall(0)
    hand_out(0, f)
    loads["gain1"].wait()
    loads["gate1"].wait()
    gate_one = fold_wide(0, 0)
    loads["up1"].wait()
    up_one = fold_wide(1, 0)
    loads["down2"].wait()
    tall_two = fold_tall(1)
    loads["gain2"].wait()
    loads["gate2"].wait()
    gate_two = fold_wide(2, 1)
    loads["up2"].wait()
    up_two = fold_wide(3, 1)
    loads["x"].wait()

    def norm(src):
        def one(k, _):
            rows = rows_of(k * 32, 32, 32)
            v = src[rows, :].astype(F32)
            scale = lax.rsqrt(jnp.mean(v * v, axis=-1, keepdims=True) + EPS)
            normed[rows, :] = (v * scale).astype(BF16)
            return 0

        lax.fori_loop(0, tokens // 32, one, 0)

    norm(x)
    tall_one.wait_recv()
    hand_out(0, other)
    hand_out(1, f)

    def hide(layer):
        gate, up = served.at[2 * layer], served.at[2 * layer + 1]
        step = tokens // 2

        def one(k, _):
            rows = rows_of(k * step, step, step)
            v = normed[rows, :]
            g = jnp.dot(v, gate[...], preferred_element_type=F32)
            u = jnp.dot(v, up[...], preferred_element_type=F32)
            hidden[rows, :] = (g / (1.0 + jnp.exp(-g)) * u).astype(BF16)
            return 0

        lax.fori_loop(0, 2, one, 0)

    def project(layer):
        step = tokens // 2

        def one(k, _):
            rows = rows_of(k * step, step, step)
            p = jnp.dot(hidden[rows, :], down[layer], preferred_element_type=F32)
            part[layer, rows, :] = p.astype(BF16)
            return 0

        lax.fori_loop(0, 2, one, 0)

    def chip_copy(src, dst, send, recv, q, sem_at, layer):
        return pltpu.make_async_remote_copy(
            src_ref=src, dst_ref=dst, send_sem=send.at[layer, q], recv_sem=recv.at[layer, sem_at],
            device_id={"fs": f, "tp": 2 * q + core}, device_id_type=MESH,
        )

    def to_sibling(src, dst, send, recv, layer):
        return pltpu.make_async_remote_copy(
            src_ref=src, dst_ref=dst, send_sem=send.at[layer], recv_sem=recv.at[layer],
            device_id={"fs": f, "tp": sibling}, device_id_type=MESH,
        )

    def scatter_copy(layer, q, sender):
        return chip_copy(
            half.at[layer, rows_of(q * piece, piece, piece)], scatter.at[layer, sender],
            s_send, s_recv, q, sender, layer,
        )

    mine = rows_of(core * side + chip * piece, piece, piece)

    def gather_copy(layer, q, sender):
        ref = rows_out.at[layer, mine]
        return chip_copy(ref, ref, g_send, g_recv, q, sender, layer)

    def for_chips(act):
        def one(k, _):
            act(lax.rem(chip + k, chips))
            return 0

        lax.fori_loop(1, chips, one, 0)

    def add_up(layer, base, between):
        swap = to_sibling(
            part.at[layer, rows_of((1 - core) * side, side, side)], pair.at[layer], p_send, p_recv, layer
        )
        swap.start()
        swap.wait_recv()

        def add(k, _):
            rows = rows_of(k * piece, piece, piece)
            own = part[layer, rows_of(core * side + k * piece, piece, piece), :].astype(F32)
            half[layer, rows, :] = (own + pair[layer, rows, :].astype(F32)).astype(BF16)
            return 0

        lax.fori_loop(0, chips, add, 0)
        for_chips(lambda q: scatter_copy(layer, q, chip).start())
        for_chips(lambda q: scatter_copy(layer, chip, q).wait_recv())
        scatter[layer, chip] = half[layer, rows_of(chip * piece, piece, piece), :]
        total = scatter[layer, 0].astype(F32)
        for q in range(1, chips):
            total = total + scatter[layer, q].astype(F32)
        rows_out[layer, mine, :] = (base[mine, :].astype(F32) + 0.5 * total).astype(BF16)
        for_chips(lambda q: gather_copy(layer, q, chip).start())
        between()
        for_chips(lambda q: gather_copy(layer, chip, q).wait_recv())
        ref = rows_out.at[layer, rows_of(core * side, side, side)]
        fill = to_sibling(ref, ref, h_send, h_recv, layer)
        fill.start()
        fill.wait_recv()
        sends.extend((swap, fill))

    gate_one.wait_recv()
    up_one.wait_recv()
    put(served.at[0], gate1_out)
    put(served.at[1], up1_out)
    hide(0)
    collect(0)
    put(down.at[0], down1_out)
    project(0)

    def relay():
        tall_two.wait_recv()
        hand_out(1, other)

    add_up(0, x, relay)
    norm(rows_out.at[0])
    gate_two.wait_recv()
    up_two.wait_recv()
    put(served.at[2], gate2_out)
    put(served.at[3], up2_out)
    hide(1)
    collect(1)
    put(down.at[1], down2_out)
    project(1)
    add_up(1, rows_out.at[0], lambda: None)
    put(rows_out.at[1], mixed_hbm)

    for sent in (tall_one, gate_one, up_one, tall_two, gate_two, up_two, *sends):
        sent.wait_send()
    for layer in range(2):

        def drain(k, _):
            block_copy(layer, lax.rem(t + k, n_tp), t).wait_send()
            return 0

        lax.fori_loop(1, n_tp, drain, 0)
        for_chips(lambda q: scatter_copy(layer, q, chip).wait_send())
        for_chips(lambda q: gather_copy(layer, q, chip).wait_send())
    for copy in outs:
        copy.wait()


def fused(n_tp, x, gain1, gate1, up1, down1, gain2, gate2, up2, down2):
    depth, width = gate1.shape
    tall_half, col = down1.shape
    tokens, model = x.shape
    block = 2 * tall_half // n_tp
    chips = n_tp // 2
    side = tokens // 2
    dma = pltpu.SemaphoreType.DMA
    shape = jax.ShapeDtypeStruct
    anywhere = pl.BlockSpec(memory_space=pl.ANY)
    wide_out = shape((2 * depth, width), BF16)
    down_out = shape((block, model), BF16)
    return pl.pallas_call(
        functools.partial(kernel, n_tp),
        out_shape=(shape(x.shape, BF16), wide_out, wide_out, down_out, wide_out, wide_out, down_out),
        in_specs=[anywhere] * 9,
        out_specs=[anywhere] * 7,
        scratch_shapes=[
            pltpu.VMEM((tokens, model), BF16),
            pltpu.VMEM((2, depth, 1), F32),
            pltpu.VMEM((4, depth, width), F32),
            pltpu.VMEM((2, tall_half, col), F32),
            pltpu.VMEM((4, 2 * depth, width), BF16),
            pltpu.VMEM((2, 2 * tall_half, col), BF16),
            pltpu.VMEM((2, block, model), BF16),
            pltpu.VMEM((tokens, model), BF16),
            pltpu.VMEM((tokens, width), BF16),
            pltpu.VMEM((2, tokens, model), BF16),
            pltpu.VMEM((2, side, model), BF16),
            pltpu.VMEM((2, side, model), BF16),
            pltpu.VMEM((2, chips, side // chips, model), BF16),
            pltpu.VMEM((2, tokens, model), BF16),
            dma((9,)), dma((7,)), dma((6,)), dma((6,)), dma((2, n_tp)), dma((2, n_tp)),
            dma((2,)), dma((2,)), dma((2, chips)), dma((2, chips)), dma((2, chips)), dma((2, chips)),
            dma((2,)), dma((2,)),
        ],
        compiler_params=pltpu.CompilerParams(
            collective_id=0, has_side_effects=True, vmem_limit_bytes=56 * 1024 * 1024
        ),
        name="hand_over",
    )(x, gain1[:, None], gate1, up1, down1, gain2[:, None], gate2, up2, down2)


def solution(mesh):
    placed = (
        P(("grp", "fs"), None),
        P("fs"),
        P("fs", "tp"),
        P("fs", "tp"),
        P("fs", "tp"),
        P("fs"),
        P("fs", "tp"),
        P("fs", "tp"),
        P("fs", "tp"),
    )
    paired = mesh.shape["fs"] == 2 and mesh.shape["tp"] % 4 == 0
    return jax.shard_map(
        functools.partial(fused, mesh.shape["tp"]) if paired else body,
        mesh=mesh,
        in_specs=placed,
        out_specs=(
            P(("grp", "fs"), None),
            P("grp", "tp"),
            P("grp", "tp"),
            P(("grp", "tp"), None),
            P("grp", "tp"),
            P("grp", "tp"),
            P(("grp", "tp"), None),
        ),
        check_vma=False,
    )
```

```python
import functools

import jax
import jax.numpy as jnp
from jax import lax
from jax.experimental import pallas as pl
from jax.experimental.pallas import tpu as pltpu
from jax.sharding import PartitionSpec as P

MESH = pl.DeviceIdType.MESH
BF16 = jnp.bfloat16
F32 = jnp.float32

EPS = 1e-06


def serve_weights(gain, gate_w, up_w, down_w):
    gate_half = (gain[:, None] * gate_w).astype(jnp.bfloat16)
    up_half = (gain[:, None] * up_w).astype(jnp.bfloat16)
    down_half = down_w.astype(jnp.bfloat16)
    gate_whole, up_whole = (
        lax.all_gather(gate_half, "fs", axis=0, tiled=True),
        lax.all_gather(up_half, "fs", axis=0, tiled=True),
    )
    tall_block = lax.all_gather(down_half, "fs", axis=0, tiled=True)
    down_whole = lax.all_to_all(tall_block, "tp", split_axis=0, concat_axis=1, tiled=True)
    return (gate_whole, up_whole, down_whole)


def half_step(row_block, gate_w, up_w, down_w):
    values = row_block.astype(jnp.float32)
    normed = (values * lax.rsqrt(jnp.mean(values * values, axis=-1, keepdims=True) + EPS)).astype(
        jnp.bfloat16
    )
    gate_pre = jnp.dot(normed, gate_w, preferred_element_type=jnp.float32)
    up_pre = jnp.dot(normed, up_w, preferred_element_type=jnp.float32)
    hidden = (jax.nn.silu(gate_pre) * up_pre).astype(jnp.bfloat16)
    total = lax.psum(
        jnp.dot(hidden, down_w, preferred_element_type=jnp.float32).astype(jnp.bfloat16), "tp"
    ).astype(jnp.float32)
    return (values + 0.5 * total).astype(jnp.bfloat16)


def body(
    prompt_rows,
    gain_before,
    gate_before,
    up_before,
    down_before,
    gain_after,
    gate_after,
    up_after,
    down_after,
):
    gate_one, up_one, down_one = serve_weights(gain_before, gate_before, up_before, down_before)
    gate_two, up_two, down_two = serve_weights(gain_after, gate_after, up_after, down_after)
    middle = half_step(prompt_rows, gate_one, up_one, down_one)
    mixed = half_step(middle, gate_two, up_two, down_two)
    return (mixed, gate_one, up_one, down_one, gate_two, up_two, down_two)


def rows_of(start, size, unit):
    return pl.ds(pl.multiple_of(start, unit), size)


def kernel(
    n_tp,
    x_hbm, gain1_hbm, gate1_hbm, up1_hbm, down1_hbm, gain2_hbm, gate2_hbm, up2_hbm, down2_hbm,
    mixed_hbm, gate1_out, up1_out, down1_out, gate2_out, up2_out, down2_out,
    x, gain, wide, tall_in, served, tall, down, normed, hidden, part, pair, half, scatter, rows_out,
    in_sem, out_sem, x_send, x_recv, a_send, a_recv, p_send, p_recv, s_send, s_recv, g_send, g_recv,
    h_send, h_recv,
):
    f = lax.axis_index("fs")
    t = lax.axis_index("tp")
    other = 1 - f
    core = lax.rem(t, 2)
    chip = t // 2
    sibling = t + 1 - 2 * core
    chips = n_tp // 2
    width, depth = wide.shape[1:]
    tall_half = tall_in.shape[1]
    block = down.shape[1]
    col = tall.shape[2]
    tokens = x.shape[0]
    side = tokens // 2
    piece = side // chips
    per_half = n_tp // 2

    loads = {}
    sources = (
        ("down1", down1_hbm, tall_in.at[0]), ("gain1", gain1_hbm, gain.at[0]),
        ("gate1", gate1_hbm, wide.at[0]), ("up1", up1_hbm, wide.at[1]),
        ("down2", down2_hbm, tall_in.at[1]), ("gain2", gain2_hbm, gain.at[1]),
        ("gate2", gate2_hbm, wide.at[2]), ("up2", up2_hbm, wide.at[3]), ("x", x_hbm, x),
    )
    for i, (name, src, dst) in enumerate(sources):
        loads[name] = pltpu.make_async_copy(src, dst, in_sem.at[i])
        loads[name].start()

    barrier = pltpu.get_barrier_semaphore()
    for k in range(1, n_tp):
        pl.semaphore_signal(
            barrier, inc=1, device_id={"fs": f, "tp": lax.rem(t + k, n_tp)}, device_id_type=MESH
        )
    pl.semaphore_signal(barrier, inc=1, device_id={"fs": other, "tp": t}, device_id_type=MESH)
    pl.semaphore_wait(barrier, n_tp)

    def across(ref, slot):
        return pltpu.make_async_remote_copy(
            src_ref=ref, dst_ref=ref, send_sem=x_send.at[slot], recv_sem=x_recv.at[slot],
            device_id={"fs": other, "tp": t}, device_id_type=MESH,
        )

    near = rows_of(f * depth, depth, depth)

    def fold_wide(i, gain_slot):
        def one(k, _):
            rows = rows_of(k * 32, 32, 32)
            served[i, rows, near] = (gain[gain_slot] * wide[i, rows, :]).astype(BF16)
            return 0

        lax.fori_loop(0, width // 32, one, 0)
        return across(served.at[i, :, near], i)

    def fold_tall(layer):
        step = tall_half // 8

        def one(k, _):
            tall[layer, rows_of(f * tall_half + k * step, step, 16), :] = tall_in[
                layer, rows_of(k * step, step, 16), :
            ].astype(BF16)
            return 0

        lax.fori_loop(0, 8, one, 0)
        return across(tall.at[layer, rows_of(f * tall_half, tall_half, 16)], 4 + layer)

    my_cols = pl.ds(pl.multiple_of(t * col, col), col)

    def block_copy(layer, b, sender):
        return pltpu.make_async_remote_copy(
            src_ref=tall.at[layer, rows_of(b * block, block, 16)],
            dst_ref=down.at[layer, :, my_cols],
            send_sem=a_send.at[layer, b], recv_sem=a_recv.at[layer, sender],
            device_id={"fs": f, "tp": b}, device_id_type=MESH,
        )

    def hand_out(layer, which):
        def one(k, _):
            b = which * per_half + lax.rem(t + k, per_half)

            @pl.when(b != t)
            def _():
                block_copy(layer, b, t).start()

            return 0

        lax.fori_loop(0, per_half, one, 0)

    def collect(layer):
        def one(k, _):
            block_copy(layer, t, lax.rem(t + k, n_tp)).wait_recv()
            return 0

        lax.fori_loop(1, n_tp, one, 0)
        down[layer, :, my_cols] = tall[layer, rows_of(t * block, block, 16), :]

    outs = []

    def put(src, dst):
        copy = pltpu.make_async_copy(src, dst, out_sem.at[len(outs)])
        copy.start()
        outs.append(copy)

    sends = []
    loads["down1"].wait()
    tall_one = fold_tall(0)
    tall_one.start()
    hand_out(0, f)
    loads["down2"].wait()
    tall_two = fold_tall(1)
    tall_two.start()
    hand_out(1, f)
    loads["gain1"].wait()
    loads["gate1"].wait()
    gate_one = fold_wide(0, 0)
    loads["up1"].wait()
    up_one = fold_wide(1, 0)
    loads["gain2"].wait()
    loads["gate2"].wait()
    gate_two = fold_wide(2, 1)
    loads["up2"].wait()
    up_two = fold_wide(3, 1)
    loads["x"].wait()

    def norm(src):
        def one(k, _):
            rows = rows_of(k * 32, 32, 32)
            v = src[rows, :].astype(F32)
            scale = lax.rsqrt(jnp.mean(v * v, axis=-1, keepdims=True) + EPS)
            normed[rows, :] = (v * scale).astype(BF16)
            return 0

        lax.fori_loop(0, tokens // 32, one, 0)

    norm(x)
    tall_one.wait_recv()
    gate_one.start()
    hand_out(0, other)
    tall_two.wait_recv()
    up_one.start()
    hand_out(1, other)

    turned = (((1,), (1,)), ((), ()))

    def hide(layer):
        gate, up = served.at[2 * layer], served.at[2 * layer + 1]
        step = tokens // 2

        def one(k, _):
            rows = rows_of(k * step, step, step)
            v = normed[rows, :]
            g = lax.dot_general(v, gate[...], turned, preferred_element_type=F32)
            u = lax.dot_general(v, up[...], turned, preferred_element_type=F32)
            hidden[rows, :] = (g / (1.0 + jnp.exp(-g)) * u).astype(BF16)
            return 0

        lax.fori_loop(0, 2, one, 0)

    def project(layer):
        step = tokens // 2

        def one(k, _):
            rows = rows_of(k * step, step, step)
            p = jnp.dot(hidden[rows, :], down[layer], preferred_element_type=F32)
            part[layer, rows, :] = p.astype(BF16)
            return 0

        lax.fori_loop(0, 2, one, 0)

    def chip_copy(src, dst, send, recv, q, sem_at, layer):
        return pltpu.make_async_remote_copy(
            src_ref=src, dst_ref=dst, send_sem=send.at[layer, q], recv_sem=recv.at[layer, sem_at],
            device_id={"fs": f, "tp": 2 * q + core}, device_id_type=MESH,
        )

    def to_sibling(src, dst, send, recv, layer):
        return pltpu.make_async_remote_copy(
            src_ref=src, dst_ref=dst, send_sem=send.at[layer], recv_sem=recv.at[layer],
            device_id={"fs": f, "tp": sibling}, device_id_type=MESH,
        )

    def scatter_copy(layer, q, sender):
        return chip_copy(
            half.at[layer, rows_of(q * piece, piece, piece)], scatter.at[layer, sender],
            s_send, s_recv, q, sender, layer,
        )

    mine = rows_of(core * side + chip * piece, piece, piece)

    def gather_copy(layer, q, sender):
        ref = rows_out.at[layer, mine]
        return chip_copy(ref, ref, g_send, g_recv, q, sender, layer)

    def for_chips(act):
        def one(k, _):
            act(lax.rem(chip + k, chips))
            return 0

        lax.fori_loop(1, chips, one, 0)

    def add_up(layer, base):
        swap = to_sibling(
            part.at[layer, rows_of((1 - core) * side, side, side)], pair.at[layer], p_send, p_recv, layer
        )
        swap.start()
        swap.wait_recv()

        def add(k, _):
            rows = rows_of(k * piece, piece, piece)
            own = part[layer, rows_of(core * side + k * piece, piece, piece), :].astype(F32)
            half[layer, rows, :] = (own + pair[layer, rows, :].astype(F32)).astype(BF16)
            return 0

        lax.fori_loop(0, chips, add, 0)
        for_chips(lambda q: scatter_copy(layer, q, chip).start())
        for_chips(lambda q: scatter_copy(layer, chip, q).wait_recv())
        scatter[layer, chip] = half[layer, rows_of(chip * piece, piece, piece), :]
        total = scatter[layer, 0].astype(F32)
        for q in range(1, chips):
            total = total + scatter[layer, q].astype(F32)
        rows_out[layer, mine, :] = (base[mine, :].astype(F32) + 0.5 * total).astype(BF16)
        for_chips(lambda q: gather_copy(layer, q, chip).start())
        for_chips(lambda q: gather_copy(layer, chip, q).wait_recv())
        ref = rows_out.at[layer, rows_of(core * side, side, side)]
        fill = to_sibling(ref, ref, h_send, h_recv, layer)
        fill.start()
        fill.wait_recv()
        sends.extend((swap, fill))

    gate_one.wait_recv()
    gate_two.start()
    put(served.at[0], gate1_out)
    up_one.wait_recv()
    up_two.start()
    put(served.at[1], up1_out)
    hide(0)
    collect(0)
    put(down.at[0], down1_out)
    project(0)
    add_up(0, x)
    norm(rows_out.at[0])
    gate_two.wait_recv()
    up_two.wait_recv()
    put(served.at[2], gate2_out)
    put(served.at[3], up2_out)
    hide(1)
    collect(1)
    put(down.at[1], down2_out)
    project(1)
    add_up(1, rows_out.at[0])
    put(rows_out.at[1], mixed_hbm)

    for sent in (tall_one, gate_one, up_one, tall_two, gate_two, up_two, *sends):
        sent.wait_send()
    for layer in range(2):

        def drain(k, _):
            block_copy(layer, lax.rem(t + k, n_tp), t).wait_send()
            return 0

        lax.fori_loop(1, n_tp, drain, 0)
        for_chips(lambda q: scatter_copy(layer, q, chip).wait_send())
        for_chips(lambda q: gather_copy(layer, q, chip).wait_send())
    for copy in outs:
        copy.wait()


def fused(n_tp, x, gain1, gate1, up1, down1, gain2, gate2, up2, down2):
    depth, width = gate1.shape
    tall_half, col = down1.shape
    tokens, model = x.shape
    block = 2 * tall_half // n_tp
    chips = n_tp // 2
    side = tokens // 2
    dma = pltpu.SemaphoreType.DMA
    shape = jax.ShapeDtypeStruct
    anywhere = pl.BlockSpec(memory_space=pl.ANY)
    wide_out = shape((width, 2 * depth), BF16)
    down_out = shape((block, model), BF16)
    mixed, gate_one, up_one, down_one, gate_two, up_two, down_two = pl.pallas_call(
        functools.partial(kernel, n_tp),
        out_shape=(shape(x.shape, BF16), wide_out, wide_out, down_out, wide_out, wide_out, down_out),
        in_specs=[anywhere] * 9,
        out_specs=[anywhere] * 7,
        scratch_shapes=[
            pltpu.VMEM((tokens, model), BF16),
            pltpu.VMEM((2, 1, depth), F32),
            pltpu.VMEM((4, width, depth), F32),
            pltpu.VMEM((2, tall_half, col), F32),
            pltpu.VMEM((4, width, 2 * depth), BF16),
            pltpu.VMEM((2, 2 * tall_half, col), BF16),
            pltpu.VMEM((2, block, model), BF16),
            pltpu.VMEM((tokens, model), BF16),
            pltpu.VMEM((tokens, width), BF16),
            pltpu.VMEM((2, tokens, model), BF16),
            pltpu.VMEM((2, side, model), BF16),
            pltpu.VMEM((2, side, model), BF16),
            pltpu.VMEM((2, chips, side // chips, model), BF16),
            pltpu.VMEM((2, tokens, model), BF16),
            dma((9,)), dma((7,)), dma((6,)), dma((6,)), dma((2, n_tp)), dma((2, n_tp)),
            dma((2,)), dma((2,)), dma((2, chips)), dma((2, chips)), dma((2, chips)), dma((2, chips)),
            dma((2,)), dma((2,)),
        ],
        compiler_params=pltpu.CompilerParams(
            collective_id=0, has_side_effects=True, vmem_limit_bytes=56 * 1024 * 1024
        ),
        name="hand_over",
    )(x, gain1[None, :], gate1.T, up1.T, down1, gain2[None, :], gate2.T, up2.T, down2)
    return (mixed, gate_one.T, up_one.T, down_one, gate_two.T, up_two.T, down_two)


def solution(mesh):
    placed = (
        P(("grp", "fs"), None),
        P("fs"),
        P("fs", "tp"),
        P("fs", "tp"),
        P("fs", "tp"),
        P("fs"),
        P("fs", "tp"),
        P("fs", "tp"),
        P("fs", "tp"),
    )
    paired = mesh.shape["fs"] == 2 and mesh.shape["tp"] % 4 == 0
    return jax.shard_map(
        functools.partial(fused, mesh.shape["tp"]) if paired else body,
        mesh=mesh,
        in_specs=placed,
        out_specs=(
            P(("grp", "fs"), None),
            P("grp", "tp"),
            P("grp", "tp"),
            P(("grp", "tp"), None),
            P("grp", "tp"),
            P("grp", "tp"),
            P(("grp", "tp"), None),
        ),
        check_vma=False,
    )
```

```python
import functools

import jax
import jax.numpy as jnp
from jax import lax
from jax.experimental import pallas as pl
from jax.experimental.pallas import tpu as pltpu
from jax.sharding import PartitionSpec as P

MESH = pl.DeviceIdType.MESH
BF16 = jnp.bfloat16
F32 = jnp.float32

EPS = 1e-06


def serve_weights(gain, gate_w, up_w, down_w):
    gate_half = (gain[:, None] * gate_w).astype(jnp.bfloat16)
    up_half = (gain[:, None] * up_w).astype(jnp.bfloat16)
    down_half = down_w.astype(jnp.bfloat16)
    gate_whole, up_whole = (
        lax.all_gather(gate_half, "fs", axis=0, tiled=True),
        lax.all_gather(up_half, "fs", axis=0, tiled=True),
    )
    tall_block = lax.all_gather(down_half, "fs", axis=0, tiled=True)
    down_whole = lax.all_to_all(tall_block, "tp", split_axis=0, concat_axis=1, tiled=True)
    return (gate_whole, up_whole, down_whole)


def half_step(row_block, gate_w, up_w, down_w):
    values = row_block.astype(jnp.float32)
    normed = (values * lax.rsqrt(jnp.mean(values * values, axis=-1, keepdims=True) + EPS)).astype(
        jnp.bfloat16
    )
    gate_pre = jnp.dot(normed, gate_w, preferred_element_type=jnp.float32)
    up_pre = jnp.dot(normed, up_w, preferred_element_type=jnp.float32)
    hidden = (jax.nn.silu(gate_pre) * up_pre).astype(jnp.bfloat16)
    total = lax.psum(
        jnp.dot(hidden, down_w, preferred_element_type=jnp.float32).astype(jnp.bfloat16), "tp"
    ).astype(jnp.float32)
    return (values + 0.5 * total).astype(jnp.bfloat16)


def body(
    prompt_rows,
    gain_before,
    gate_before,
    up_before,
    down_before,
    gain_after,
    gate_after,
    up_after,
    down_after,
):
    gate_one, up_one, down_one = serve_weights(gain_before, gate_before, up_before, down_before)
    gate_two, up_two, down_two = serve_weights(gain_after, gate_after, up_after, down_after)
    middle = half_step(prompt_rows, gate_one, up_one, down_one)
    mixed = half_step(middle, gate_two, up_two, down_two)
    return (mixed, gate_one, up_one, down_one, gate_two, up_two, down_two)


def rows_of(start, size, unit):
    return pl.ds(pl.multiple_of(start, unit), size)


def kernel(
    n_tp,
    x_hbm, gain1_hbm, gate1_hbm, up1_hbm, down1_hbm, gain2_hbm, gate2_hbm, up2_hbm, down2_hbm,
    mixed_hbm, gate1_out, up1_out, down1_out, gate2_out, up2_out, down2_out,
    x, gain, wide, tall_in, served, tall, down, normed, hidden, part, pair, half, scatter, rows_out,
    in_sem, out_sem, x_send, x_recv, a_send, a_recv, p_send, p_recv, s_send, s_recv, g_send, g_recv,
    h_send, h_recv,
):
    f = lax.axis_index("fs")
    t = lax.axis_index("tp")
    other = 1 - f
    core = lax.rem(t, 2)
    chip = t // 2
    sibling = t + 1 - 2 * core
    chips = n_tp // 2
    width, depth = wide.shape[1:]
    tall_half = tall_in.shape[1]
    block = down.shape[1]
    col = tall.shape[2]
    tokens = x.shape[0]
    side = tokens // 2
    piece = side // chips
    per_half = n_tp // 2

    loads = {}
    sources = (
        ("down1", down1_hbm, tall_in.at[0]), ("gain1", gain1_hbm, gain.at[0]),
        ("gate1", gate1_hbm, wide.at[0]), ("up1", up1_hbm, wide.at[1]),
        ("down2", down2_hbm, tall_in.at[1]), ("gain2", gain2_hbm, gain.at[1]),
        ("gate2", gate2_hbm, wide.at[2]), ("up2", up2_hbm, wide.at[3]), ("x", x_hbm, x),
    )
    for i, (name, src, dst) in enumerate(sources):
        loads[name] = pltpu.make_async_copy(src, dst, in_sem.at[i])
        loads[name].start()

    barrier = pltpu.get_barrier_semaphore()
    for k in range(1, n_tp):
        pl.semaphore_signal(
            barrier, inc=1, device_id={"fs": f, "tp": lax.rem(t + k, n_tp)}, device_id_type=MESH
        )
    pl.semaphore_signal(barrier, inc=1, device_id={"fs": other, "tp": t}, device_id_type=MESH)
    pl.semaphore_wait(barrier, n_tp)

    def across(ref, slot):
        return pltpu.make_async_remote_copy(
            src_ref=ref, dst_ref=ref, send_sem=x_send.at[slot], recv_sem=x_recv.at[slot],
            device_id={"fs": other, "tp": t}, device_id_type=MESH,
        )

    near = rows_of(f * depth, depth, depth)

    def fold_wide(i, gain_slot):
        def one(k, _):
            rows = rows_of(k * 32, 32, 32)
            served[i, rows, near] = (gain[gain_slot] * wide[i, rows, :]).astype(BF16)
            return 0

        lax.fori_loop(0, width // 32, one, 0)
        return across(served.at[i, :, near], i)

    def fold_tall(layer):
        step = tall_half // 8

        def one(k, _):
            tall[layer, rows_of(f * tall_half + k * step, step, 16), :] = tall_in[
                layer, rows_of(k * step, step, 16), :
            ].astype(BF16)
            return 0

        lax.fori_loop(0, 8, one, 0)
        return across(tall.at[layer, rows_of(f * tall_half, tall_half, 16)], 4 + layer)

    my_cols = pl.ds(pl.multiple_of(t * col, col), col)

    def block_copy(layer, b, sender):
        return pltpu.make_async_remote_copy(
            src_ref=tall.at[layer, rows_of(b * block, block, 16)],
            dst_ref=down.at[layer, :, my_cols],
            send_sem=a_send.at[layer, b], recv_sem=a_recv.at[layer, sender],
            device_id={"fs": f, "tp": b}, device_id_type=MESH,
        )

    def hand_out(layer, which):
        def one(k, _):
            b = which * per_half + lax.rem(t + k, per_half)

            @pl.when(b != t)
            def _():
                block_copy(layer, b, t).start()

            return 0

        lax.fori_loop(0, per_half, one, 0)

    def collect(layer):
        def one(k, _):
            block_copy(layer, t, lax.rem(t + k, n_tp)).wait_recv()
            return 0

        lax.fori_loop(1, n_tp, one, 0)
        down[layer, :, my_cols] = tall[layer, rows_of(t * block, block, 16), :]

    outs = []

    def put(src, dst):
        copy = pltpu.make_async_copy(src, dst, out_sem.at[len(outs)])
        copy.start()
        outs.append(copy)

    sends = []
    loads["down1"].wait()
    tall_one = fold_tall(0)
    tall_one.start()
    hand_out(0, f)
    loads["down2"].wait()
    tall_two = fold_tall(1)
    tall_two.start()
    hand_out(1, f)
    loads["gain1"].wait()
    loads["gate1"].wait()
    gate_one = fold_wide(0, 0)
    loads["up1"].wait()
    up_one = fold_wide(1, 0)
    loads["gain2"].wait()
    loads["gate2"].wait()
    gate_two = fold_wide(2, 1)
    loads["up2"].wait()
    up_two = fold_wide(3, 1)
    loads["x"].wait()

    def norm(src):
        def one(k, _):
            rows = rows_of(k * 32, 32, 32)
            v = src[rows, :].astype(F32)
            scale = lax.rsqrt(jnp.mean(v * v, axis=-1, keepdims=True) + EPS)
            normed[rows, :] = (v * scale).astype(BF16)
            return 0

        lax.fori_loop(0, tokens // 32, one, 0)

    norm(x)
    tall_one.wait_recv()
    gate_one.start()
    hand_out(0, other)
    tall_two.wait_recv()
    up_one.start()
    hand_out(1, other)

    turned = (((1,), (1,)), ((), ()))

    def hide(layer):
        gate, up = served.at[2 * layer], served.at[2 * layer + 1]
        step = tokens // 2

        def one(k, _):
            rows = rows_of(k * step, step, step)
            v = normed[rows, :]
            g = lax.dot_general(v, gate[...], turned, preferred_element_type=F32)
            u = lax.dot_general(v, up[...], turned, preferred_element_type=F32)
            hidden[rows, :] = (g / (1.0 + jnp.exp(-g)) * u).astype(BF16)
            return 0

        lax.fori_loop(0, 2, one, 0)

    def project(layer):
        step = tokens // 2

        def one(k, _):
            rows = rows_of(k * step, step, step)
            p = jnp.dot(hidden[rows, :], down[layer], preferred_element_type=F32)
            part[layer, rows, :] = p.astype(BF16)
            return 0

        lax.fori_loop(0, 2, one, 0)

    def chip_copy(src, dst, send, recv, q, sem_at, layer):
        return pltpu.make_async_remote_copy(
            src_ref=src, dst_ref=dst, send_sem=send.at[layer, q], recv_sem=recv.at[layer, sem_at],
            device_id={"fs": f, "tp": 2 * q + core}, device_id_type=MESH,
        )

    def to_sibling(src, dst, send, recv, layer):
        return pltpu.make_async_remote_copy(
            src_ref=src, dst_ref=dst, send_sem=send.at[layer], recv_sem=recv.at[layer],
            device_id={"fs": f, "tp": sibling}, device_id_type=MESH,
        )

    lanes = chips // 2
    lane = lax.rem(chip, 2)
    beside = chip + 1 - 2 * lane

    def place(q):
        return lax.rem(q, 2) * lanes + q // 2

    def scatter_copy(layer, q, sender):
        return chip_copy(
            half.at[layer, rows_of(place(q) * piece, piece, piece)], scatter.at[layer, sender],
            s_send, s_recv, q, sender, layer,
        )

    mine = rows_of(core * side + place(chip) * piece, piece, piece)

    def gather_copy(layer, q, sender):
        ref = rows_out.at[layer, mine]
        return chip_copy(ref, ref, g_send, g_recv, q, sender, layer)

    def for_chips(act):
        def one(k, _):
            act(lax.rem(chip + k, chips))
            return 0

        lax.fori_loop(1, chips, one, 0)

    def for_lane(act):
        def one(k, _):
            act(2 * lax.rem(chip // 2 + k, lanes) + lane)
            return 0

        lax.fori_loop(1, lanes, one, 0)

    def beside_copy(layer, sender):
        ref = rows_out.at[layer, rows_of(core * side + lane * (side // 2), side // 2, side // 2)]
        return chip_copy(ref, ref, g_send, g_recv, beside, sender, layer)

    def add_up(layer, base):
        swap = to_sibling(
            part.at[layer, rows_of((1 - core) * side, side, side)], pair.at[layer], p_send, p_recv, layer
        )
        swap.start()
        swap.wait_recv()

        def add(k, _):
            rows = rows_of(k * piece, piece, piece)
            own = part[layer, rows_of(core * side + k * piece, piece, piece), :].astype(F32)
            half[layer, rows, :] = (own + pair[layer, rows, :].astype(F32)).astype(BF16)
            return 0

        lax.fori_loop(0, chips, add, 0)
        for_chips(lambda q: scatter_copy(layer, q, chip).start())
        for_chips(lambda q: scatter_copy(layer, chip, q).wait_recv())
        scatter[layer, chip] = half[layer, rows_of(place(chip) * piece, piece, piece), :]
        total = scatter[layer, 0].astype(F32)
        for q in range(1, chips):
            total = total + scatter[layer, q].astype(F32)
        rows_out[layer, mine, :] = (base[mine, :].astype(F32) + 0.5 * total).astype(BF16)
        spread = for_chips if layer else for_lane
        spread(lambda q: gather_copy(layer, q, chip).start())
        spread(lambda q: gather_copy(layer, chip, q).wait_recv())
        if layer == 0:
            beside_copy(layer, chip).start()
            beside_copy(layer, beside).wait_recv()
        ref = rows_out.at[layer, rows_of(core * side, side, side)]
        fill = to_sibling(ref, ref, h_send, h_recv, layer)
        fill.start()
        fill.wait_recv()
        sends.extend((swap, fill))

    gate_one.wait_recv()
    gate_two.start()
    put(served.at[0], gate1_out)
    up_one.wait_recv()
    up_two.start()
    put(served.at[1], up1_out)
    hide(0)
    collect(0)
    put(down.at[0], down1_out)
    project(0)
    add_up(0, x)
    norm(rows_out.at[0])
    gate_two.wait_recv()
    up_two.wait_recv()
    put(served.at[2], gate2_out)
    put(served.at[3], up2_out)
    hide(1)
    collect(1)
    put(down.at[1], down2_out)
    project(1)
    add_up(1, rows_out.at[0])
    put(rows_out.at[1], mixed_hbm)

    for sent in (tall_one, gate_one, up_one, tall_two, gate_two, up_two, *sends):
        sent.wait_send()
    for layer in range(2):

        def drain(k, _):
            block_copy(layer, lax.rem(t + k, n_tp), t).wait_send()
            return 0

        lax.fori_loop(1, n_tp, drain, 0)
        for_chips(lambda q: scatter_copy(layer, q, chip).wait_send())
        if layer == 0:
            for_lane(lambda q: gather_copy(layer, q, chip).wait_send())
            beside_copy(layer, chip).wait_send()
        else:
            for_chips(lambda q: gather_copy(layer, q, chip).wait_send())
    for copy in outs:
        copy.wait()


def fused(n_tp, x, gain1, gate1, up1, down1, gain2, gate2, up2, down2):
    depth, width = gate1.shape
    tall_half, col = down1.shape
    tokens, model = x.shape
    block = 2 * tall_half // n_tp
    chips = n_tp // 2
    side = tokens // 2
    dma = pltpu.SemaphoreType.DMA
    shape = jax.ShapeDtypeStruct
    anywhere = pl.BlockSpec(memory_space=pl.ANY)
    wide_out = shape((width, 2 * depth), BF16)
    down_out = shape((block, model), BF16)
    mixed, gate_one, up_one, down_one, gate_two, up_two, down_two = pl.pallas_call(
        functools.partial(kernel, n_tp),
        out_shape=(shape(x.shape, BF16), wide_out, wide_out, down_out, wide_out, wide_out, down_out),
        in_specs=[anywhere] * 9,
        out_specs=[anywhere] * 7,
        scratch_shapes=[
            pltpu.VMEM((tokens, model), BF16),
            pltpu.VMEM((2, 1, depth), F32),
            pltpu.VMEM((4, width, depth), F32),
            pltpu.VMEM((2, tall_half, col), F32),
            pltpu.VMEM((4, width, 2 * depth), BF16),
            pltpu.VMEM((2, 2 * tall_half, col), BF16),
            pltpu.VMEM((2, block, model), BF16),
            pltpu.VMEM((tokens, model), BF16),
            pltpu.VMEM((tokens, width), BF16),
            pltpu.VMEM((2, tokens, model), BF16),
            pltpu.VMEM((2, side, model), BF16),
            pltpu.VMEM((2, side, model), BF16),
            pltpu.VMEM((2, chips, side // chips, model), BF16),
            pltpu.VMEM((2, tokens, model), BF16),
            dma((9,)), dma((7,)), dma((6,)), dma((6,)), dma((2, n_tp)), dma((2, n_tp)),
            dma((2,)), dma((2,)), dma((2, chips)), dma((2, chips)), dma((2, chips)), dma((2, chips)),
            dma((2,)), dma((2,)),
        ],
        compiler_params=pltpu.CompilerParams(
            collective_id=0, has_side_effects=True, vmem_limit_bytes=56 * 1024 * 1024
        ),
        name="hand_over",
    )(x, gain1[None, :], gate1.T, up1.T, down1, gain2[None, :], gate2.T, up2.T, down2)
    return (mixed, gate_one.T, up_one.T, down_one, gate_two.T, up_two.T, down_two)


def solution(mesh):
    placed = (
        P(("grp", "fs"), None),
        P("fs"),
        P("fs", "tp"),
        P("fs", "tp"),
        P("fs", "tp"),
        P("fs"),
        P("fs", "tp"),
        P("fs", "tp"),
        P("fs", "tp"),
    )
    paired = mesh.shape["fs"] == 2 and mesh.shape["tp"] % 4 == 0
    return jax.shard_map(
        functools.partial(fused, mesh.shape["tp"]) if paired else body,
        mesh=mesh,
        in_specs=placed,
        out_specs=(
            P(("grp", "fs"), None),
            P("grp", "tp"),
            P("grp", "tp"),
            P(("grp", "tp"), None),
            P("grp", "tp"),
            P("grp", "tp"),
            P(("grp", "tp"), None),
        ),
        check_vma=False,
    )
```
